32 devices in a mesh: ep: 8 (over z, core), tp: 4 (over y, x).
Axes of the slice: x: 2, y: 2, z: 4, core: 2. Of those that a mesh axis runs over, the one named last changes fastest.
Arguments:
- query_rows: bfloat16 [3072, 2048], P('ep', 'tp'), may hold values from -6 to 6
- key_rows: bfloat16 [3072, 2048], P('ep', 'tp'), may hold values from -6 to 6
- value_rows: bfloat16 [3072, 2048], P('ep', 'tp'), may hold values from -6 to 6
- second_scale: float32 [16], P('tp'), may hold values from 0.3 to 0.8
- head_gain: float32 [128], replicated, may hold values from 0.1 to 1.9
- out_weight: bfloat16 [2048, 4096], P(None, 'tp'), may hold values from -0.125 to 0.125
- routed_rows: bfloat16 [1024, 4096], P('ep', 'tp'), may hold values from -6 to 6
- norm_gain: float32 [4096], replicated, may hold values from 0.1 to 1.9
- route_ids: int32 [1024, 2], P('ep'), may hold values from 0 to 7, all different within a row; in each aligned block of 128 rows (0 to 127, 128 to 255, ...) at most 64 rows name the same one
- route_weight: float32 [1024, 2], P('ep'), may hold values from 0.1 to 0.9
- expert_gate: bfloat16 [8, 4096, 2048], P('ep', None, 'tp'), may hold values from -0.09375 to 0.09375
- expert_up: bfloat16 [8, 4096, 2048], P('ep', None, 'tp'), may hold values from -0.09375 to 0.09375
- expert_down: bfloat16 [8, 2048, 4096], P('ep', None, 'tp'), may hold values from -0.125 to 0.125
Outputs:
- mixer_out: bfloat16 [3072, 4096], P('ep', 'tp')
- expert_mix: bfloat16 [1024, 4096], P('ep', 'tp')
The draws below stay inside these ranges and needn't reach their ends.
Inputs may be any that keep to these rules, and one draw needn't show every extreme that they name: `route_ids`: among the 128 tokens of one index of ep, no expert is named by more than 64 of them, a bound that some block reaches.
All inputs are finite; a program needn't handle non-finite values.
Results may differ from the reference program's by a relative error of at most 0.0085.
Values may be sent and summed in bfloat16 or wider, within the bound.
A program may use at most 128 MiB of HBM per device.

```python
import math
import jax
import jax.numpy as jnp
import numpy as np
from jax import lax

D = 4096
HEADS = 16
HD = 64
VD = 128
FF = 2048
TOP = 2
TOK_A = 384
TOK_B = 128
TOKENS_A = 3072
TOKENS_B = 1024
EXPERTS = 8
CAP = 64
N_EP = 8


def draw_query_rows(key, part):
    length_all = TOK_A * N_EP
    drawn_rows = jnp.clip(1.3 * jax.random.normal(jax.random.fold_in(key, 3), (length_all, HEADS * 2 * HD), jnp.float32), -6.0, 6.0)
    return drawn_rows.astype(jnp.bfloat16)


def draw_key_rows(key, part):
    length_all = TOK_A * N_EP
    drawn_rows = jnp.clip(1.3 * jax.random.normal(jax.random.fold_in(key, 5), (length_all, HEADS * 2 * HD), jnp.float32), -6.0, 6.0)
    return drawn_rows.astype(jnp.bfloat16)


def level_of(rng, shape, split, smallest, largest):
    factor_of = 1.0
    for axis_at, parts in split:
        draws = jax.random.uniform(jax.random.fold_in(jax.random.fold_in(rng, 6), axis_at), (parts,), jnp.float32, smallest / len(split), largest / len(split))
        factor_of = factor_of * jnp.repeat(jnp.exp(draws), shape[axis_at] // parts).reshape((-1,) + (1,) * (len(shape) - 1 - axis_at))
    return factor_of


def deal_out(stream_key, own, number, rows, number_of, top, bound, slope):
    order = jax.random.permutation(stream_key, number_of)
    crowded, ordinary = load_shares(number_of, rows * top, bound, slope, True), load_shares(number_of, rows * top, bound, slope, False)
    places = jnp.arange(number_of)

    def named(sizes, offset_by):
        used = int((sizes > 0).sum())
        fixed = max(1, used // 4)
        passed = fixed + (places - fixed + offset_by * (used - fixed)) % max(1, number_of - fixed)
        return jnp.zeros((number_of,), jnp.int32).at[order[jnp.where(places < fixed, places, passed)]].set(jnp.asarray(sizes, jnp.int32))

    sizes = jnp.where(number % 4 == 0, named(crowded, number // 4), named(ordinary, number - number // 4 - 1))
    mixed = jax.random.permutation(jax.random.fold_in(own, 3), number_of)
    giver, sink = mixed[0:number_of // 2 * 2:2], mixed[1:number_of // 2 * 2:2]
    margin = jnp.minimum(sizes[giver] - 1, bound - sizes[sink]) // 2
    margin = jnp.where((giver == order[0]) | (sink == order[0]) | (sizes[sink] == 0), 0, jnp.maximum(margin, 0))
    passed = jax.random.randint(jax.random.fold_in(own, 4), (number_of // 2,), 0, 1 << 20) % (margin + 1)
    sizes = sizes.at[giver].add(-passed).at[sink].add(passed)
    labels = jnp.searchsorted(jnp.cumsum(sizes), jnp.arange(rows * top), side="right").astype(jnp.int32)
    table = labels.reshape(top, rows).T
    table = table[jax.random.permutation(jax.random.fold_in(own, 1), rows)]
    offset_by = jax.random.randint(jax.random.fold_in(own, 2), (rows, 1), 0, top)
    return jnp.take_along_axis(table, (jnp.arange(top)[None, :] + offset_by) % top, axis=1)


def load_shares(amount, total, limit, slope, full):
    loads = [(1 << 20) // math.isqrt(rank ** slope) + 1 for rank in range(1, amount + 1)]
    largest = limit if full else min(limit, max(-(-total // amount), total * loads[0] // sum(loads)))
    least = 1 if total - largest >= amount - 1 else 0
    given, spare = [largest] + [least] * (amount - 1), total - largest - least * (amount - 1)
    while spare > 0:
        free = [i for i in range(1, amount) if given[i] < largest] or [i for i in range(1, amount) if given[i] < limit]
        pool, remaining = sum([loads[i] for i in free]), spare
        for i in free:
            more = min(limit - given[i], max(1, remaining * loads[i] // pool), spare)
            given[i] = given[i] + more
            spare = spare - more
    return np.array(given)


def normal_values(key, dims, spread, reach, pieces=(), held_as=jnp.bfloat16):
    level = level_of(key, dims, pieces, -0.22, 0.18) if pieces else 1.0
    values = jax.random.normal(key, dims, jnp.float32) * spread * level
    return jnp.minimum(jnp.maximum(values, -reach), reach).astype(held_as)


def setup_inputs(seed: int = 0) -> dict:
    keys = jax.random.split(jax.random.key(seed), 14)
    query_rows = draw_query_rows(jax.random.fold_in(keys[13], 71), 0)
    key_rows = draw_key_rows(jax.random.fold_in(keys[13], 71), 0)
    value_rows = normal_values(keys[2], (TOKENS_A, HEADS * VD), 1.0, 6.0, ((0, 8), (1, 4)))
    second_scale = jnp.clip(0.3 + 0.5 * jax.random.uniform(keys[3], (HEADS,), jnp.float32) ** level_of(keys[3], (HEADS,), ((0, 4),), -0.2, 0.2), 0.3, 0.8)
    head_gain = jnp.clip(1.0 + 0.18 * jax.random.normal(keys[4], (VD,), jnp.float32), 0.1, 1.9)
    out_weight = normal_values(keys[5], (HEADS * VD, D), (HEADS * VD) ** -0.5, 0.125, ((1, 4),))
    routed_rows = normal_values(keys[6], (TOKENS_B, D), 1.0, 6.0, ((0, 8), (1, 4)))
    norm_gain = jnp.clip(1.0 + 0.18 * jax.random.normal(keys[7], (D,), jnp.float32), 0.1, 1.9)
    route_ids_keys = jax.random.split(jax.random.fold_in(keys[8], 1), TOKENS_B // TOK_B)
    route_ids_turns = jax.random.permutation(jax.random.fold_in(keys[8], 3), TOKENS_B // TOK_B)
    route_ids = jax.vmap(lambda own, number: deal_out(jax.random.fold_in(keys[8], 2), own, number, TOK_B, EXPERTS, TOP, CAP, 1))(route_ids_keys, route_ids_turns).reshape((TOKENS_B, TOP))
    route_weight = jnp.clip(0.1 + 0.79999997 * jax.random.uniform(keys[9], (TOKENS_B, TOP), jnp.float32) ** level_of(keys[9], (TOKENS_B, TOP), ((0, 8),), -0.2, 0.2), 0.1, 0.9)
    expert_gate = normal_values(keys[10], (EXPERTS, D, FF), D ** -0.5, 0.09375, ((0, 8), (2, 4)))
    expert_up = normal_values(keys[11], (EXPERTS, D, FF), D ** -0.5, 0.09375, ((0, 8), (2, 4)))
    expert_down = normal_values(keys[12], (EXPERTS, FF, D), FF ** -0.5, 0.125, ((0, 8), (2, 4)))
    return {"query_rows": query_rows, "key_rows": key_rows, "value_rows": value_rows, "second_scale": second_scale, "head_gain": head_gain, "out_weight": out_weight, "routed_rows": routed_rows, "norm_gain": norm_gain, "route_ids": route_ids, "route_weight": route_weight, "expert_gate": expert_gate, "expert_up": expert_up, "expert_down": expert_down}


eps = 1e-06
head_factor = 0.8
neg_big = -1e+30

def rms_rows(rows_in, gain):
    floats = rows_in.astype(jnp.float32)
    factor = lax.rsqrt(lax.optimization_barrier(jnp.mean(floats * floats, axis=-1, keepdims=True)) + eps)
    return (floats * factor * gain).astype(jnp.bfloat16)

def reference(query_rows, key_rows, value_rows, second_scale, head_gain, out_weight, routed_rows, norm_gain, route_ids, route_weight, expert_gate, expert_up, expert_down):
    length_all = query_rows.shape[0]
    block_rows = min(512, length_all)
    positions = jnp.arange(length_all, dtype=jnp.int32)
    query_heads = jnp.transpose(query_rows.reshape(length_all, HEADS, 2, HD), (1, 0, 2, 3))
    key_heads = jnp.transpose(key_rows.reshape(length_all, HEADS, 2, HD), (1, 0, 2, 3))
    value_heads = jnp.transpose(value_rows.reshape(length_all, HEADS, VD), (1, 0, 2))

    def one_head(operands):
        query_h, key_h, value_h, scale_h = operands
        key_float = key_h.astype(jnp.float32)
        value_float = value_h.astype(jnp.float32)

        def one_block(block_num):
            row_first = block_num * block_rows
            query_block = lax.dynamic_slice_in_dim(query_h, row_first, block_rows, 0).astype(jnp.float32)
            scores = jnp.einsum('icd,jcd->cij', query_block, key_float) * HD ** (-0.5)
            allowed = ((row_first + jnp.arange(block_rows, dtype=jnp.int32))[:, None] >= positions[None, :])[None]
            scores = jnp.where(allowed, scores, neg_big)
            row_max = lax.optimization_barrier(jnp.max(scores, axis=-1, keepdims=True))
            exp_scores = jnp.where(allowed, jnp.exp(scores - row_max), 0.0)
            denoms = lax.optimization_barrier(jnp.sum(exp_scores, axis=-1))
            rounded = lax.optimization_barrier(exp_scores.astype(jnp.bfloat16)).astype(jnp.float32)
            maps_both = jnp.einsum('cij,je->cie', rounded, value_float) / denoms[..., None]
            mixed_maps = maps_both[0] - scale_h * maps_both[1]
            mean_sq = lax.optimization_barrier(jnp.mean(mixed_maps * mixed_maps, axis=-1, keepdims=True))
            return (mixed_maps * lax.rsqrt(mean_sq + eps) * head_gain * head_factor).astype(jnp.bfloat16)
        block_outs = lax.map(one_block, jnp.arange(length_all // block_rows, dtype=jnp.int32))
        return block_outs.reshape(length_all, VD)
    head_outs = lax.map(one_head, (query_heads, key_heads, value_heads, second_scale))
    head_cat = jnp.transpose(head_outs, (1, 0, 2)).reshape(length_all, HEADS * VD)
    mixer_out = jnp.dot(head_cat, out_weight, preferred_element_type=jnp.float32).astype(jnp.bfloat16)
    normed = rms_rows(routed_rows, norm_gain)
    flat_expert = route_ids.reshape(-1).astype(jnp.int32)
    count_all = flat_expert.shape[0]
    chosen = (flat_expert[:, None] == jnp.arange(EXPERTS, dtype=jnp.int32)[None, :]).astype(jnp.int32)
    ranks = lax.optimization_barrier(jnp.sum((jnp.cumsum(chosen, axis=0) - 1) * chosen, axis=1)).astype(jnp.int32)
    token_of = jnp.arange(count_all, dtype=jnp.int32) // TOP
    table = jnp.full((EXPERTS, N_EP * CAP), TOKENS_B, jnp.int32).at[flat_expert, ranks].set(token_of)
    padded = jnp.concatenate([normed, jnp.zeros((1, D), jnp.bfloat16)], axis=0)

    def one_expert(operands):
        table_row, gate_w, up_w, down_w = operands
        gathered = padded[table_row]
        gate_val = jnp.dot(gathered, gate_w, preferred_element_type=jnp.float32)
        up_val = jnp.dot(gathered, up_w, preferred_element_type=jnp.float32)
        hidden = (jax.nn.silu(gate_val) * up_val).astype(jnp.bfloat16)
        return jnp.dot(hidden, down_w, preferred_element_type=jnp.float32).astype(jnp.bfloat16)
    expert_outs = lax.map(one_expert, (table, expert_gate, expert_up, expert_down))
    picked = expert_outs[flat_expert, ranks].astype(jnp.float32).reshape(TOKENS_B, TOP, D)
    expert_mix = lax.optimization_barrier(jnp.sum(picked * route_weight[:, :, None], axis=1)).astype(jnp.bfloat16)
    return (mixer_out, expert_mix)
```

```python
import functools

import jax
import jax.numpy as jnp
from jax import lax
from jax.experimental import pallas as pl
from jax.experimental.pallas import tpu as pltpu
from jax.sharding import PartitionSpec as P

eps = 1e-06
head_factor = 0.8
neg_big = -1e30
lanes = 2
f32 = jnp.float32
bf16 = jnp.bfloat16


def dot(a, b):
    return jnp.dot(a, b, preferred_element_type=f32)


def layer_kernel(
    n_ep,
    n_tp,
    scale_ref,
    q_hbm,
    k_hbm,
    v_hbm,
    gain_ref,
    wo_hbm,
    rows_hbm,
    norm_ref,
    ids_row_hbm,
    ids_col_ref,
    route_w_ref,
    wg_hbm,
    wu_hbm,
    wd_hbm,
    mixer_ref,
    mix_ref,
    q_in,
    q_two,
    k_all,
    v_all,
    rows_all,
    ids_all,
    arr,
    normed,
    hid_all,
    out_e,
    ret,
    head_all,
    acc,
    run_max,
    run_sum,
    wg,
    wu,
    wd,
    wo,
    local_sem,
    weight_sem,
    rows_up,
    rows_down,
    rows_side,
    rows_recv,
    ids_send,
    ids_recv,
    kv_up,
    kv_side,
    kv_recv,
    arr_send,
    arr_recv,
    hid_send,
    hid_recv,
    head_send,
    head_recv,
    ret_send,
    ret_recv,
):
    e = lax.axis_index("ep")
    t = lax.axis_index("tp")
    n_z = n_ep // lanes
    z = lax.div(e, lanes)
    c = lax.rem(e, lanes)
    partner = z * lanes + (1 - c)
    n_tok = q_in.shape[0]
    tok_b = rows_all.shape[1]
    per_head = acc.shape[0]
    head_w = q_two.shape[2]
    val_w = acc.shape[2]
    cap = ret.shape[1]
    slots = n_ep * cap
    cols = arr.shape[2]
    hidden_w = hid_all.shape[2]
    route_count = ids_col_ref.shape[1]

    def remote(src, dst, send, recv, ep_to, tp_to):
        return pltpu.make_async_remote_copy(
            src_ref=src,
            dst_ref=dst,
            send_sem=send,
            recv_sem=recv,
            device_id=(ep_to, tp_to),
            device_id_type=pl.DeviceIdType.MESH,
        )

    loads = [
        pltpu.make_async_copy(rows_hbm, rows_all.at[e], local_sem.at[0]),
        pltpu.make_async_copy(ids_row_hbm, ids_all.at[e], local_sem.at[1]),
        pltpu.make_async_copy(k_hbm, k_all.at[e], local_sem.at[2]),
        pltpu.make_async_copy(v_hbm, v_all.at[e], local_sem.at[3]),
        pltpu.make_async_copy(q_hbm, q_in, local_sem.at[4]),
    ]
    for load in loads:
        load.start()
    weights = [
        pltpu.make_async_copy(wg_hbm.at[0], wg, weight_sem.at[0]),
        pltpu.make_async_copy(wu_hbm.at[0], wu, weight_sem.at[1]),
        pltpu.make_async_copy(wd_hbm.at[0], wd, weight_sem.at[2]),
        pltpu.make_async_copy(wo_hbm, wo, weight_sem.at[3]),
    ]

    barrier = pltpu.get_barrier_semaphore()

    def greet_ep(i, carry):
        to = lax.rem(e + i, n_ep)
        pl.semaphore_signal(barrier, inc=1, device_id=(to, t), device_id_type=pl.DeviceIdType.MESH)
        return carry

    def greet_tp(i, carry):
        to = lax.rem(t + i, n_tp)
        pl.semaphore_signal(barrier, inc=1, device_id=(e, to), device_id_type=pl.DeviceIdType.MESH)
        return carry

    lax.fori_loop(1, n_ep, greet_ep, 0)
    lax.fori_loop(1, n_tp, greet_tp, 0)
    pl.semaphore_wait(barrier, n_ep - 1 + n_tp - 1)
    for load in loads:
        load.wait()

    def ids_copy(to):
        return remote(ids_all.at[e], ids_all.at[e], ids_send.at[to], ids_recv.at[e], to, t)

    def ids_arrival(b):
        return remote(ids_all.at[b], ids_all.at[b], ids_send.at[b], ids_recv.at[b], b, t)

    def rows_copy(block, send, to):
        return remote(rows_all.at[block], rows_all.at[block], send, rows_recv.at[block], to, t)

    def rows_copy_up(j):
        return rows_copy(j * lanes + c, rows_up.at[j], lax.rem(e + lanes, n_ep))

    def rows_copy_down(j):
        return rows_copy(j * lanes + c, rows_down.at[j], lax.rem(e + n_ep - lanes, n_ep))

    def rows_copy_side(j):
        return rows_copy(j * lanes + c, rows_side.at[j], partner)

    def kv_copies(j, sems, to):
        block = j * lanes + c
        return [
            remote(ref.at[block], ref.at[block], sems.at[i, j], kv_recv.at[i, block], to, t)
            for i, ref in enumerate((k_all, v_all))
        ]

    def kv_copies_up(j):
        return kv_copies(j, kv_up, lax.rem(e + lanes, n_ep))

    def kv_copies_side(j):
        return kv_copies(j, kv_side, partner)

    def kv_wait(block):
        for i, ref in enumerate((k_all, v_all)):
            remote(
                ref.at[block], ref.at[block], kv_up.at[i, 0], kv_recv.at[i, block], partner, t
            ).wait_recv()

    def arr_piece(block):
        return arr.at[t, pl.ds(pl.multiple_of(block * cap, cap), cap)]

    def tp_copy(buf, send, recv, source, to):
        return remote(buf.at[source], buf.at[source], send.at[to], recv.at[source], e, to)

    def tp_send_all(buf, send, recv):
        def one(i, carry):
            tp_copy(buf, send, recv, t, lax.rem(t + i, n_tp)).start()
            return carry

        lax.fori_loop(1, n_tp, one, 0)

    def tp_wait_recv(buf, send, recv):
        def one(i, carry):
            other = lax.rem(t + i, n_tp)
            tp_copy(buf, send, recv, other, other).wait_recv()
            return carry

        lax.fori_loop(1, n_tp, one, 0)

    def tp_wait_send(buf, send, recv):
        def one(i, carry):
            tp_copy(buf, send, recv, t, lax.rem(t + i, n_tp)).wait_send()
            return carry

        lax.fori_loop(1, n_tp, one, 0)

    def ret_copy(to):
        return remote(
            out_e.at[pl.ds(pl.multiple_of(to * cap, cap), cap)],
            ret.at[e],
            ret_send.at[to],
            ret_recv.at[e],
            to,
            t,
        )

    def ret_arrival(b):
        return remote(ret.at[b], ret.at[b], ret_send.at[b], ret_recv.at[b], b, t)

    def each_ep(work):
        def one(i, carry):
            work(lax.rem(e + i, n_ep))
            return carry

        lax.fori_loop(1, n_ep, one, 0)

    each_ep(lambda to: ids_copy(to).start())

    def pick(block):
        ids = ids_all[block]
        hit = (ids[0:1] == e).astype(f32)
        for k in range(1, route_count):
            hit = hit + (ids[k : k + 1] == e).astype(f32)
        before = (
            lax.broadcasted_iota(jnp.int32, (tok_b, tok_b), 0)
            < lax.broadcasted_iota(jnp.int32, (tok_b, tok_b), 1)
        ).astype(bf16)
        ranks = dot(jnp.broadcast_to(hit, (16, tok_b)).astype(bf16), before)[0:1]
        slot = lax.broadcasted_iota(jnp.int32, (cap, tok_b), 0).astype(f32)
        chosen = jnp.where((slot == ranks) & (hit > 0.5), 1.0, 0.0).astype(bf16)
        start = pl.multiple_of(block * cap, cap)
        arr[t, pl.ds(start, cap)] = dot(chosen, rows_all[block]).astype(bf16)

        def one(i, carry):
            to = lax.rem(t + i, n_tp)
            remote(arr_piece(block), arr_piece(block), arr_send.at[to], arr_recv.at[t], e, to).start()
            return carry

        lax.fori_loop(1, n_tp, one, 0)

    def rows_step(s, carry):
        low, high = z - s, z + s

        @pl.when((s > 0) & (low >= 0))
        def _():
            rows_copy_down(low).wait_recv()

        @pl.when((low >= 0) & (z + 1 < n_z))
        def _():
            rows_copy_up(low).start()

        @pl.when((s > 0) & (high < n_z))
        def _():
            rows_copy_up(high).wait_recv()

        @pl.when((high < n_z) & (z > 0))
        def _():
            rows_copy_down(high).start()

        @pl.when((s == z) & (z + 1 < n_z))
        def _():
            for copy in kv_copies_up(z):
                copy.start()

        @pl.when((s == z) & (c == 0))
        def _():
            for copy in kv_copies_side(z):
                copy.start()

        @pl.when(low >= 0)
        def _():
            rows_copy_side(low).start()

        @pl.when((s > 0) & (high < n_z))
        def _():
            rows_copy_side(high).start()

        def take(j):
            mine, other = j * lanes + c, j * lanes + (1 - c)

            @pl.when(j != z)
            def _():
                ids_arrival(mine).wait_recv()

            pick(mine)
            ids_arrival(other).wait_recv()
            rows_copy(other, rows_side.at[j], partner).wait_recv()
            pick(other)

        @pl.when(low >= 0)
        def _():
            take(low)

        @pl.when((s > 0) & (high < n_z))
        def _():
            take(high)

        return carry

    lax.fori_loop(0, n_z, rows_step, 0)
    for weight in weights:
        weight.start()

    lane = lax.broadcasted_iota(jnp.int32, (n_tok, head_w), 1)

    def split_maps(h, carry):
        scaled = q_in[:, pl.ds(pl.multiple_of(h * head_w, head_w), head_w)].astype(f32) * (
            (head_w // 2) ** -0.5
        )
        q_two[h, pl.ds(0, n_tok)] = jnp.where(lane < head_w // 2, scaled, 0.0).astype(bf16)
        q_two[h, pl.ds(n_tok, n_tok)] = jnp.where(lane < head_w // 2, 0.0, scaled).astype(bf16)
        return carry

    lax.fori_loop(0, per_head, split_maps, 0)

    def attend(block, own):
        def one(h, carry):
            keys = k_all[block, :, pl.ds(pl.multiple_of(h * head_w, head_w), head_w)]
            values = v_all[block, :, pl.ds(pl.multiple_of(h * val_w, val_w), val_w)]
            for m in range(2):
                part = pl.ds(m * n_tok, n_tok)
                scores = lax.dot_general(
                    q_two[h, part], keys, (((1,), (1,)), ((), ())), preferred_element_type=f32
                )
                if own:
                    scores = jnp.where(
                        lax.broadcasted_iota(jnp.int32, (n_tok, n_tok), 0)
                        >= lax.broadcasted_iota(jnp.int32, (n_tok, n_tok), 1),
                        scores,
                        neg_big,
                    )
                top = jnp.max(scores, axis=-1, keepdims=True)
                if not own:
                    old = run_max[h, part]
                    top = jnp.maximum(old, top)
                shares = jnp.exp(scores - top)
                total = jnp.sum(shares, axis=-1, keepdims=True)
                update = dot(shares.astype(bf16), values)
                if not own:
                    shrink = jnp.exp(old - top)
                    total = total + run_sum[h, part] * shrink
                    update = update + acc[h, part] * shrink
                run_max[h, part] = top
                run_sum[h, part] = total
                acc[h, part] = update
            return carry

        lax.fori_loop(0, per_head, one, 0)

    attend(e, True)

    @pl.when(c == 1)
    def _():
        kv_wait(partner)
        attend(partner, False)

    def kv_step(s, carry):
        j = z - s

        @pl.when(j >= 0)
        def _():
            kv_wait(j * lanes + c)

            @pl.when(z + 1 < n_z)
            def _():
                for copy in kv_copies_up(j):
                    copy.start()

            for copy in kv_copies_side(j):
                copy.start()
            attend(j * lanes + c, False)
            kv_wait(j * lanes + (1 - c))
            attend(j * lanes + (1 - c), False)

        return carry

    lax.fori_loop(1, n_z - 1, kv_step, 0)

    def arr_wait(i, carry):
        other = lax.rem(t + i, n_tp)
        tp_copy(arr, arr_send, arr_recv, other, other).wait_recv()
        return carry

    lax.fori_loop(1, n_tp, arr_wait, 0)
    for weight in weights:
        weight.wait()
    n_rows = min(slots, 64)

    def norm_step(i, carry):
        part = pl.ds(pl.multiple_of(i * n_rows, n_rows), n_rows)
        squares = jnp.zeros((n_rows, 1), f32)
        for p in range(n_tp):
            x = arr[p, part].astype(f32)
            squares = squares + jnp.sum(x * x, axis=-1, keepdims=True)
        factor = lax.rsqrt(squares / (n_tp * cols) + eps)
        for p in range(n_tp):
            where = pl.ds(p * cols, cols)
            normed[part, where] = (
                arr[p, part].astype(f32) * factor * norm_ref[0:1, where]
            ).astype(bf16)
        return carry

    lax.fori_loop(0, slots // n_rows, norm_step, 0)
    tile_f = min(hidden_w, 256)

    def gate_step(i, carry):
        where = pl.ds(pl.multiple_of(i * tile_f, tile_f), tile_f)
        gate = dot(normed[...], wg[:, where])
        up = dot(normed[...], wu[:, where])
        hid_all[t, :, where] = (gate / (1.0 + jnp.exp(-gate)) * up).astype(bf16)
        return carry

    lax.fori_loop(0, hidden_w // tile_f, gate_step, 0)
    tp_send_all(hid_all, hid_send, hid_recv)

    lax.fori_loop(n_z - 1, n_z, kv_step, 0)

    def head_step(h, carry):
        first = acc[h, pl.ds(0, n_tok)] / run_sum[h, pl.ds(0, n_tok)]
        second = acc[h, pl.ds(n_tok, n_tok)] / run_sum[h, pl.ds(n_tok, n_tok)]
        mixed = first - scale_ref[h] * second
        mean_sq = jnp.mean(mixed * mixed, axis=-1, keepdims=True)
        head_all[t, :, pl.ds(pl.multiple_of(h * val_w, val_w), val_w)] = (
            mixed * lax.rsqrt(mean_sq + eps) * gain_ref[0:1] * head_factor
        ).astype(bf16)
        return carry

    lax.fori_loop(0, per_head, head_step, 0)
    tp_send_all(head_all, head_send, head_recv)

    tp_wait_recv(hid_all, hid_send, hid_recv)
    out_w = out_e.shape[1]
    tile_o = min(out_w, 256)

    def down_step(i, carry):
        where = pl.ds(pl.multiple_of(i * tile_o, tile_o), tile_o)
        total = dot(hid_all[0], wd[pl.ds(0, hidden_w), where])
        for p in range(1, n_tp):
            total = total + dot(hid_all[p], wd[pl.ds(p * hidden_w, hidden_w), where])
        out_e[:, where] = total.astype(bf16)
        return carry

    lax.fori_loop(0, out_w // tile_o, down_step, 0)
    each_ep(lambda to: ret_copy(to).start())
    ret[e] = out_e[pl.ds(pl.multiple_of(e * cap, cap), cap)]

    tp_wait_recv(head_all, head_send, head_recv)
    heads_w = head_all.shape[2]

    def mixer_step(i, carry):
        where = pl.ds(pl.multiple_of(i * tile_o, tile_o), tile_o)
        total = dot(head_all[0], wo[pl.ds(0, heads_w), where])
        for p in range(1, n_tp):
            total = total + dot(head_all[p], wo[pl.ds(p * heads_w, heads_w), where])
        mixer_ref[:, where] = total.astype(bf16)
        return carry

    lax.fori_loop(0, out_w // tile_o, mixer_step, 0)

    each_ep(lambda b: ret_arrival(b).wait_recv())
    after = (
        lax.broadcasted_iota(jnp.int32, (tok_b, tok_b), 0)
        > lax.broadcasted_iota(jnp.int32, (tok_b, tok_b), 1)
    ).astype(bf16)

    def mix_step(b, total):
        hit = jnp.zeros((tok_b, 1), f32)
        share = jnp.zeros((tok_b, 1), f32)
        for k in range(route_count):
            named = ids_col_ref[:, k : k + 1] == b
            hit = hit + named.astype(f32)
            share = share + jnp.where(named, route_w_ref[:, k : k + 1], 0.0)
        ranks = dot(after, jnp.broadcast_to(hit, (tok_b, tok_b)).astype(bf16))[:, :cap]
        slot = lax.broadcasted_iota(jnp.int32, (tok_b, cap), 1).astype(f32)
        chosen = jnp.where((slot == ranks) & (hit > 0.5), 1.0, 0.0).astype(bf16)
        return total + share * dot(chosen, ret[b])

    mix_ref[...] = lax.fori_loop(0, n_ep, mix_step, jnp.zeros((tok_b, out_w), f32)).astype(bf16)

    each_ep(lambda to: ids_copy(to).wait_send())
    each_ep(lambda to: ret_copy(to).wait_send())
    tp_wait_send(arr, arr_send, arr_recv)
    tp_wait_send(hid_all, hid_send, hid_recv)
    tp_wait_send(head_all, head_send, head_recv)

    def drain(j, carry):
        rows_copy_side(j).wait_send()

        @pl.when((j <= z) & (z + 1 < n_z))
        def _():
            rows_copy_up(j).wait_send()
            for copy in kv_copies_up(j):
                copy.wait_send()

        @pl.when((j >= z) & (z > 0))
        def _():
            rows_copy_down(j).wait_send()

        @pl.when((j < z) | ((j == z) & (c == 0)))
        def _():
            for copy in kv_copies_side(j):
                copy.wait_send()

        return carry

    lax.fori_loop(0, n_z, drain, 0)


def per_device(
    n_ep,
    n_tp,
    query_rows,
    key_rows,
    value_rows,
    second_scale,
    head_gain,
    out_weight,
    routed_rows,
    norm_gain,
    route_ids,
    route_weight,
    expert_gate,
    expert_up,
    expert_down,
):
    n_tok, attn_w = query_rows.shape
    per_head = second_scale.shape[0]
    val_w = head_gain.shape[0]
    head_w = attn_w // per_head
    tok_b, cols = routed_rows.shape
    route_count = route_ids.shape[1]
    hidden_w = expert_gate.shape[2]
    out_w = out_weight.shape[1]
    n_z = n_ep // lanes
    cap = 2 * tok_b * route_count // n_ep
    slots = n_ep * cap
    ids_row = jnp.pad(route_ids.T, ((0, 8 - route_count), (0, 0)))
    vmem = pl.BlockSpec(memory_space=pltpu.VMEM)
    hbm = pl.BlockSpec(memory_space=pl.ANY)
    dma = pltpu.SemaphoreType.DMA
    return pl.pallas_call(
        functools.partial(layer_kernel, n_ep, n_tp),
        out_shape=(
            jax.ShapeDtypeStruct((n_tok, out_w), bf16),
            jax.ShapeDtypeStruct((tok_b, out_w), bf16),
        ),
        in_specs=[
            pl.BlockSpec(memory_space=pltpu.SMEM),
            hbm,
            hbm,
            hbm,
            vmem,
            hbm,
            hbm,
            vmem,
            hbm,
            vmem,
            vmem,
            hbm,
            hbm,
            hbm,
        ],
        out_specs=(vmem, vmem),
        scratch_shapes=[
            pltpu.VMEM((n_tok, attn_w), bf16),
            pltpu.VMEM((per_head, 2 * n_tok, head_w), bf16),
            pltpu.VMEM((n_ep, n_tok, attn_w), bf16),
            pltpu.VMEM((n_ep, n_tok, value_rows.shape[1]), bf16),
            pltpu.VMEM((n_ep, tok_b, cols), bf16),
            pltpu.VMEM((n_ep, 8, tok_b), jnp.int32),
            pltpu.VMEM((n_tp, slots, cols), bf16),
            pltpu.VMEM((slots, n_tp * cols), bf16),
            pltpu.VMEM((n_tp, slots, hidden_w), bf16),
            pltpu.VMEM((slots, out_w), bf16),
            pltpu.VMEM((n_ep, cap, out_w), bf16),
            pltpu.VMEM((n_tp, n_tok, per_head * val_w), bf16),
            pltpu.VMEM((per_head, 2 * n_tok, val_w), f32),
            pltpu.VMEM((per_head, 2 * n_tok, 1), f32),
            pltpu.VMEM((per_head, 2 * n_tok, 1), f32),
            pltpu.VMEM(expert_gate.shape[1:], bf16),
            pltpu.VMEM(expert_up.shape[1:], bf16),
            pltpu.VMEM(expert_down.shape[1:], bf16),
            pltpu.VMEM(out_weight.shape, bf16),
            dma((5,)),
            dma((4,)),
            dma((n_z,)),
            dma((n_z,)),
            dma((n_z,)),
            dma((n_ep,)),
            dma((n_ep,)),
            dma((n_ep,)),
            dma((2, n_z)),
            dma((2, n_z)),
            dma((2, n_ep)),
            dma((n_tp,)),
            dma((n_tp,)),
            dma((n_tp,)),
            dma((n_tp,)),
            dma((n_tp,)),
            dma((n_tp,)),
            dma((n_ep,)),
            dma((n_ep,)),
        ],
        compiler_params=pltpu.CompilerParams(
            collective_id=0, has_side_effects=True, vmem_limit_bytes=66000000
        ),
    )(
        second_scale,
        query_rows,
        key_rows,
        value_rows,
        head_gain.reshape(1, -1),
        out_weight,
        routed_rows,
        norm_gain.reshape(1, -1),
        ids_row,
        route_ids,
        route_weight,
        expert_gate,
        expert_up,
        expert_down,
    )


def solution(mesh):
    placed = (
        P("ep", "tp"),
        P("ep", "tp"),
        P("ep", "tp"),
        P("tp"),
        P(),
        P(None, "tp"),
        P("ep", "tp"),
        P(),
        P("ep", None),
        P("ep", None),
        P("ep", None, "tp"),
        P("ep", None, "tp"),
        P("ep", None, "tp"),
    )
    return jax.shard_map(
        functools.partial(per_device, mesh.shape["ep"], mesh.shape["tp"]),
        mesh=mesh,
        in_specs=placed,
        out_specs=(P("ep", "tp"), P("ep", "tp")),
        check_vma=False,
    )
```

```python
import functools

import jax
import jax.numpy as jnp
from jax import lax
from jax.experimental import pallas as pl
from jax.experimental.pallas import tpu as pltpu
from jax.sharding import PartitionSpec as P

eps = 1e-06
head_factor = 0.8
neg_big = -1e30
lanes = 2
f32 = jnp.float32
bf16 = jnp.bfloat16


def dot(a, b):
    return jnp.dot(a, b, preferred_element_type=f32)


def layer_kernel(
    n_ep,
    n_tp,
    scale_ref,
    q_hbm,
    k_hbm,
    v_hbm,
    gain_ref,
    wo_hbm,
    rows_hbm,
    norm_ref,
    ids_ref,
    route_w_ref,
    wg_hbm,
    wu_hbm,
    wd_hbm,
    mixer_ref,
    mix_ref,
    q_in,
    q_two,
    k_all,
    v_all,
    rows_all,
    ids_all,
    arr,
    normed,
    hid_all,
    out_e,
    ret,
    head_all,
    spread,
    acc,
    run_max,
    run_sum,
    wg,
    wu,
    wd,
    wo,
    local_sem,
    weight_sem,
    rows_up,
    rows_down,
    rows_side,
    rows_recv,
    ids_send,
    ids_recv,
    kv_up,
    kv_side,
    kv_recv,
    arr_send,
    arr_recv,
    hid_send,
    hid_recv,
    head_send,
    head_recv,
    ret_send,
    ret_recv,
):
    e = lax.axis_index("ep")
    t = lax.axis_index("tp")
    n_z = n_ep // lanes
    z = lax.div(e, lanes)
    c = lax.rem(e, lanes)
    partner = z * lanes + (1 - c)
    n_tok = q_in.shape[0]
    tok_b = rows_all.shape[1]
    per_head = acc.shape[0]
    head_w = q_two.shape[2]
    val_w = acc.shape[2]
    slots, out_w = ret.shape
    cap = slots // n_ep
    half = n_z // 2
    cols = arr.shape[2]
    hidden_w = hid_all.shape[2]
    route_count = ids_ref.shape[0]

    def remote(src, dst, send, recv, ep_to, tp_to):
        return pltpu.make_async_remote_copy(
            src_ref=src,
            dst_ref=dst,
            send_sem=send,
            recv_sem=recv,
            device_id=(ep_to, tp_to),
            device_id_type=pl.DeviceIdType.MESH,
        )

    loads = [
        pltpu.make_async_copy(rows_hbm, rows_all.at[e], local_sem.at[0]),
        pltpu.make_async_copy(k_hbm, k_all.at[e], local_sem.at[1]),
        pltpu.make_async_copy(v_hbm, v_all.at[e], local_sem.at[2]),
        pltpu.make_async_copy(q_hbm, q_in, local_sem.at[3]),
    ]
    for load in loads:
        load.start()
    ids_all[e, pl.ds(0, route_count)] = ids_ref[...]
    weights = [
        pltpu.make_async_copy(wg_hbm.at[0], wg, weight_sem.at[0]),
        pltpu.make_async_copy(wu_hbm.at[0], wu, weight_sem.at[1]),
        pltpu.make_async_copy(wd_hbm.at[0], wd, weight_sem.at[2]),
        pltpu.make_async_copy(wo_hbm, wo, weight_sem.at[3]),
    ]

    barrier = pltpu.get_barrier_semaphore()

    def greet_ep(i, carry):
        to = lax.rem(e + i, n_ep)
        pl.semaphore_signal(barrier, inc=1, device_id=(to, t), device_id_type=pl.DeviceIdType.MESH)
        return carry

    def greet_tp(i, carry):
        to = lax.rem(t + i, n_tp)
        pl.semaphore_signal(barrier, inc=1, device_id=(e, to), device_id_type=pl.DeviceIdType.MESH)
        return carry

    lax.fori_loop(1, n_ep, greet_ep, 0)
    lax.fori_loop(1, n_tp, greet_tp, 0)
    pl.semaphore_wait(barrier, n_ep - 1 + n_tp - 1)
    for load in loads:
        load.wait()

    def ids_copy(to):
        return remote(ids_all.at[e], ids_all.at[e], ids_send.at[to], ids_recv.at[e], to, t)

    def ids_arrival(b):
        return remote(ids_all.at[b], ids_all.at[b], ids_send.at[b], ids_recv.at[b], b, t)

    def rows_copy(block, send, to):
        return remote(rows_all.at[block], rows_all.at[block], send, rows_recv.at[block], to, t)

    def rows_copy_up(j):
        return rows_copy(j * lanes + c, rows_up.at[j], lax.rem(e + lanes, n_ep))

    def rows_copy_down(j):
        return rows_copy(j * lanes + c, rows_down.at[j], lax.rem(e + n_ep - lanes, n_ep))

    def rows_copy_side(j):
        return rows_copy(j * lanes + c, rows_side.at[j], partner)

    def kv_copies(j, sems, to):
        block = j * lanes + c
        return [
            remote(ref.at[block], ref.at[block], sems.at[i, j], kv_recv.at[i, block], to, t)
            for i, ref in enumerate((k_all, v_all))
        ]

    def kv_copies_up(j):
        return kv_copies(j, kv_up, lax.rem(e + lanes, n_ep))

    def kv_copies_side(j):
        return kv_copies(j, kv_side, partner)

    def kv_wait(block):
        for i, ref in enumerate((k_all, v_all)):
            remote(
                ref.at[block], ref.at[block], kv_up.at[i, 0], kv_recv.at[i, block], partner, t
            ).wait_recv()

    square = n_tp == 4
    across = t + 1 - 2 * lax.rem(t, 2)
    along = lax.rem(t + 2, n_tp)
    corner = n_tp - 1 - t

    def piece(buf, source, i, units):
        step = buf.shape[1] // (2 * units)
        return buf.at[source, pl.ds(i * step, step)]

    def tp_copy(buf, sems, units, source, i, row, to):
        ref = piece(buf, source, i, units)
        return remote(ref, ref, sems[0].at[row, i], sems[1].at[source, i], e, to)

    def tp_peers(work):
        def one(i, carry):
            to = lax.rem(t + i, n_tp)
            work(to, to)
            return carry

        if square:
            work(across, 0)
            work(along, 1)
        else:
            lax.fori_loop(1, n_tp, one, 0)

    def tp_send(buf, sems, units, unit):
        for i in (2 * unit, 2 * unit + 1):
            tp_peers(lambda to, row: tp_copy(buf, sems, units, t, i, row, to).start())

    def tp_hand_on(buf, sems, units, unit):
        if square:
            i = 2 * unit
            tp_copy(buf, sems, units, across, i, 2, across).wait_recv()
            tp_copy(buf, sems, units, across, i, 2, along).start()
            tp_copy(buf, sems, units, along, i + 1, 2, along).wait_recv()
            tp_copy(buf, sems, units, along, i + 1, 2, across).start()

    def tp_arrive(buf, sems, units, unit):
        i = 2 * unit
        if square:
            for source, at in ((across, i + 1), (along, i), (corner, i), (corner, i + 1)):
                tp_copy(buf, sems, units, source, at, 2, source).wait_recv()
        else:
            for at in (i, i + 1):
                tp_peers(lambda to, row: tp_copy(buf, sems, units, to, at, row, to).wait_recv())

    def tp_drain(buf, sems, units):
        for i in range(2 * units):
            tp_peers(lambda to, row: tp_copy(buf, sems, units, t, i, row, to).wait_send())
            if square:
                source, to = (across, along) if i % 2 == 0 else (along, across)
                tp_copy(buf, sems, units, source, i, 2, to).wait_send()

    arr_sems = (arr_send, arr_recv)
    hid_sems = (hid_send, hid_recv)
    head_sems = (head_send, head_recv)

    def unit_of(j):
        return lax.rem(lax.div(j, half) + lax.div(z, half), 2)

    def first_slot(j, side):
        return pl.multiple_of(((unit_of(j) * 2 + side) * half + lax.rem(j, half)) * cap, cap)

    def ret_part(b):
        return ret.at[pl.ds(pl.multiple_of(b * cap, cap), cap)]

    def ret_copy(j, side):
        to = j * lanes + (c if side == 0 else 1 - c)
        return remote(
            out_e.at[pl.ds(first_slot(j, side), cap)],
            ret_part(e),
            ret_send.at[to],
            ret_recv.at[e],
            to,
            t,
        )

    def ret_each(unit, work):
        def one(i, carry):
            j = lax.rem(lax.div(z, half) + unit, 2) * half + i
            if unit == 0:

                @pl.when(j != z)
                def _():
                    work(ret_copy(j, 0))

            else:
                work(ret_copy(j, 0))
            work(ret_copy(j, 1))
            return carry

        lax.fori_loop(0, half, one, 0)

    def ret_arrival(b):
        return remote(ret_part(b), ret_part(b), ret_send.at[b], ret_recv.at[b], b, t)

    def each_ep(work):
        def one(i, carry):
            work(lax.rem(e + i, n_ep))
            return carry

        lax.fori_loop(1, n_ep, one, 0)

    each_ep(lambda to: ids_copy(to).start())

    def pick(block, j, side):
        ids = ids_all[block]
        hit = (ids[0:1] == e).astype(f32)
        for k in range(1, route_count):
            hit = hit + (ids[k : k + 1] == e).astype(f32)
        before = (
            lax.broadcasted_iota(jnp.int32, (tok_b, tok_b), 0)
            < lax.broadcasted_iota(jnp.int32, (tok_b, tok_b), 1)
        ).astype(bf16)
        ranks = dot(jnp.broadcast_to(hit, (16, tok_b)).astype(bf16), before)[0:1]
        slot = lax.broadcasted_iota(jnp.int32, (cap, tok_b), 0).astype(f32)
        chosen = jnp.where((slot == ranks) & (hit > 0.5), 1.0, 0.0).astype(bf16)
        start = first_slot(j, side)
        i = unit_of(j) * 2 + side
        arr[t, pl.ds(start, cap)] = dot(chosen, rows_all[block]).astype(bf16)
        part = arr.at[t, pl.ds(start, cap)]
        tp_peers(
            lambda to, row: remote(
                part, part, arr_send.at[row, i], arr_recv.at[t, i], e, to
            ).start()
        )

    def rows_step(s, carry):
        low, high = z - s, z + s

        @pl.when((s > 0) & (low >= 0))
        def _():
            rows_copy_down(low).wait_recv()

        @pl.when((low >= 0) & (z + 1 < n_z))
        def _():
            rows_copy_up(low).start()

        @pl.when((s > 0) & (high < n_z))
        def _():
            rows_copy_up(high).wait_recv()

        @pl.when((high < n_z) & (z > 0))
        def _():
            rows_copy_down(high).start()

        @pl.when((s == z) & (z + 1 < n_z))
        def _():
            for copy in kv_copies_up(z):
                copy.start()

        @pl.when((s == z) & (c == 0))
        def _():
            for copy in kv_copies_side(z):
                copy.start()

        @pl.when(low >= 0)
        def _():
            rows_copy_side(low).start()

        @pl.when((s > 0) & (high < n_z))
        def _():
            rows_copy_side(high).start()

        def take(j):
            mine, other = j * lanes + c, j * lanes + (1 - c)

            @pl.when(j != z)
            def _():
                ids_arrival(mine).wait_recv()

            pick(mine, j, 0)
            ids_arrival(other).wait_recv()
            rows_copy(other, rows_side.at[j], partner).wait_recv()
            pick(other, j, 1)

        @pl.when(low >= 0)
        def _():
            take(low)

        @pl.when((s > 0) & (high < n_z))
        def _():
            take(high)

        return carry

    lax.fori_loop(0, n_z, rows_step, 0)
    for weight in weights:
        weight.start()
    tp_hand_on(arr, arr_sems, 2, 0)

    lane = lax.broadcasted_iota(jnp.int32, (n_tok, head_w), 1)

    def split_maps(h, carry):
        scaled = q_in[:, pl.ds(pl.multiple_of(h * head_w, head_w), head_w)].astype(f32) * (
            (head_w // 2) ** -0.5
        )
        q_two[h, pl.ds(0, n_tok)] = jnp.where(lane < head_w // 2, scaled, 0.0).astype(bf16)
        q_two[h, pl.ds(n_tok, n_tok)] = jnp.where(lane < head_w // 2, 0.0, scaled).astype(bf16)
        return carry

    lax.fori_loop(0, per_head, split_maps, 0)

    def attend(block, own):
        def one(h, carry):
            keys = k_all[block, :, pl.ds(pl.multiple_of(h * head_w, head_w), head_w)]
            values = v_all[block, :, pl.ds(pl.multiple_of(h * val_w, val_w), val_w)]
            for m in range(2):
                part = pl.ds(m * n_tok, n_tok)
                scores = lax.dot_general(
                    q_two[h, part], keys, (((1,), (1,)), ((), ())), preferred_element_type=f32
                )
                if own:
                    scores = jnp.where(
                        lax.broadcasted_iota(jnp.int32, (n_tok, n_tok), 0)
                        >= lax.broadcasted_iota(jnp.int32, (n_tok, n_tok), 1),
                        scores,
                        neg_big,
                    )
                top = jnp.max(scores, axis=-1, keepdims=True)
                if not own:
                    old = run_max[h, part]
                    top = jnp.maximum(old, top)
                shares = jnp.exp(scores - top)
                total = jnp.sum(shares, axis=-1, keepdims=True)
                update = dot(shares.astype(bf16), values)
                if not own:
                    shrink = jnp.exp(old - top)
                    total = total + run_sum[h, part] * shrink
                    update = update + acc[h, part] * shrink
                run_max[h, part] = top
                run_sum[h, part] = total
                acc[h, part] = update
            return carry

        lax.fori_loop(0, per_head, one, 0)

    attend(e, True)

    @pl.when(c == 1)
    def _():
        kv_wait(partner)
        attend(partner, False)

    tp_hand_on(arr, arr_sems, 2, 1)

    def kv_pass(s, carry):
        j = z - s

        @pl.when(j >= 0)
        def _():
            kv_wait(j * lanes + c)

            @pl.when(z + 1 < n_z)
            def _():
                for copy in kv_copies_up(j):
                    copy.start()

            for copy in kv_copies_side(j):
                copy.start()

        return carry

    def kv_attend(s, carry):
        j = z - s

        @pl.when(j >= 0)
        def _():
            attend(j * lanes + c, False)
            kv_wait(j * lanes + (1 - c))
            attend(j * lanes + (1 - c), False)

        return carry

    lax.fori_loop(1, 2, kv_pass, 0)

    for weight in weights:
        weight.wait()
    unit_rows = slots // 2
    n_rows = min(unit_rows, 64)
    tile_f = min(hidden_w, 256)

    def expert_in(unit):
        tp_arrive(arr, arr_sems, 2, unit)

        def norm_step(i, carry):
            part = pl.ds(pl.multiple_of(unit * unit_rows + i * n_rows, n_rows), n_rows)
            squares = jnp.zeros((n_rows, 1), f32)
            for p in range(n_tp):
                x = arr[p, part].astype(f32)
                squares = squares + jnp.sum(x * x, axis=-1, keepdims=True)
            factor = lax.rsqrt(squares / (n_tp * cols) + eps)
            for p in range(n_tp):
                where = pl.ds(p * cols, cols)
                normed[part, where] = (
                    arr[p, part].astype(f32) * factor * norm_ref[0:1, where]
                ).astype(bf16)
            return carry

        lax.fori_loop(0, unit_rows // n_rows, norm_step, 0)
        rows = pl.ds(unit * unit_rows, unit_rows)

        def gate_step(i, carry):
            where = pl.ds(pl.multiple_of(i * tile_f, tile_f), tile_f)
            gate = dot(normed[rows], wg[:, where])
            up = dot(normed[rows], wu[:, where])
            hid_all[t, rows, where] = (gate / (1.0 + jnp.exp(-gate)) * up).astype(bf16)
            return carry

        lax.fori_loop(0, hidden_w // tile_f, gate_step, 0)
        tp_send(hid_all, hid_sems, 2, unit)

    expert_in(0)
    expert_in(1)
    lax.fori_loop(1, 2, kv_attend, 0)

    @pl.when(z + 1 < n_z)
    def _():
        lax.fori_loop(2, n_z - 1, kv_pass, 0)

    tp_hand_on(hid_all, hid_sems, 2, 0)
    tp_hand_on(hid_all, hid_sems, 2, 1)
    tile_o = min(out_w, 256)

    def expert_out(unit):
        tp_arrive(hid_all, hid_sems, 2, unit)
        rows = pl.ds(unit * unit_rows, unit_rows)

        def down_step(i, carry):
            where = pl.ds(pl.multiple_of(i * tile_o, tile_o), tile_o)
            total = dot(hid_all[0, rows], wd[pl.ds(0, hidden_w), where])
            for p in range(1, n_tp):
                total = total + dot(hid_all[p, rows], wd[pl.ds(p * hidden_w, hidden_w), where])
            out_e[rows, where] = total.astype(bf16)
            return carry

        lax.fori_loop(0, out_w // tile_o, down_step, 0)
        ret_each(unit, lambda copy: copy.start())

    expert_out(0)
    expert_out(1)
    ret[pl.ds(pl.multiple_of(e * cap, cap), cap)] = out_e[pl.ds(first_slot(z, 0), cap)]

    def kv_late(s, carry):
        @pl.when(z + 1 == n_z)
        def _():
            kv_pass(s, 0)

        return kv_attend(s, carry)

    lax.fori_loop(2, n_z, kv_late, 0)

    def head_step(h, carry):
        first = acc[h, pl.ds(0, n_tok)] / run_sum[h, pl.ds(0, n_tok)]
        second = acc[h, pl.ds(n_tok, n_tok)] / run_sum[h, pl.ds(n_tok, n_tok)]
        mixed = first - scale_ref[h] * second
        mean_sq = jnp.mean(mixed * mixed, axis=-1, keepdims=True)
        head_all[t, :, pl.ds(pl.multiple_of(h * val_w, val_w), val_w)] = (
            mixed * lax.rsqrt(mean_sq + eps) * gain_ref[0:1] * head_factor
        ).astype(bf16)
        return carry

    lax.fori_loop(0, per_head, head_step, 0)
    tp_send(head_all, head_sems, 1, 0)

    row_of = lax.broadcasted_iota(jnp.int32, (tok_b, tok_b), 0)
    col_of = lax.broadcasted_iota(jnp.int32, (tok_b, tok_b), 1)

    def column(row):
        return jnp.sum(
            jnp.where(row_of == col_of, row.astype(f32), 0.0), axis=1, keepdims=True
        )

    shares = []
    for k in range(route_count):
        ids = column(ids_ref[k : k + 1])
        same = jnp.zeros((tok_b, tok_b), f32)
        for other in range(route_count):
            same = same + (ids_ref[other : other + 1].astype(f32) == ids).astype(f32)
        ranks = jnp.sum(jnp.where(col_of < row_of, same, 0.0), axis=1, keepdims=True)
        slot = lax.broadcasted_iota(jnp.int32, (tok_b, slots), 1).astype(f32)
        spread[k] = jnp.where(slot == ids * cap + ranks, 1.0, 0.0).astype(bf16)
        shares.append(column(route_w_ref[k : k + 1]))

    tp_hand_on(head_all, head_sems, 1, 0)
    tp_arrive(head_all, head_sems, 1, 0)
    heads_w = head_all.shape[2]

    def mixer_step(i, carry):
        where = pl.ds(pl.multiple_of(i * tile_o, tile_o), tile_o)
        total = dot(head_all[0], wo[pl.ds(0, heads_w), where])
        for p in range(1, n_tp):
            total = total + dot(head_all[p], wo[pl.ds(p * heads_w, heads_w), where])
        mixer_ref[:, where] = total.astype(bf16)
        return carry

    lax.fori_loop(0, out_w // tile_o, mixer_step, 0)

    each_ep(lambda b: ret_arrival(b).wait_recv())
    tile_m = min(out_w, 256)
    for start in range(0, out_w, tile_m):
        where = pl.ds(start, tile_m)
        total = shares[0] * dot(spread[0], ret[:, where])
        for k in range(1, route_count):
            total = total + shares[k] * dot(spread[k], ret[:, where])
        mix_ref[:, where] = total.astype(bf16)

    each_ep(lambda to: ids_copy(to).wait_send())
    for unit in range(2):
        ret_each(unit, lambda copy: copy.wait_send())
    tp_drain(arr, arr_sems, 2)
    tp_drain(hid_all, hid_sems, 2)
    tp_drain(head_all, head_sems, 1)

    def drain(j, carry):
        rows_copy_side(j).wait_send()

        @pl.when((j <= z) & (z + 1 < n_z))
        def _():
            rows_copy_up(j).wait_send()
            for copy in kv_copies_up(j):
                copy.wait_send()

        @pl.when((j >= z) & (z > 0))
        def _():
            rows_copy_down(j).wait_send()

        @pl.when((j < z) | ((j == z) & (c == 0)))
        def _():
            for copy in kv_copies_side(j):
                copy.wait_send()

        return carry

    lax.fori_loop(0, n_z, drain, 0)


def per_device(
    n_ep,
    n_tp,
    query_rows,
    key_rows,
    value_rows,
    second_scale,
    head_gain,
    out_weight,
    routed_rows,
    norm_gain,
    route_ids,
    route_weight,
    expert_gate,
    expert_up,
    expert_down,
):
    n_tok, attn_w = query_rows.shape
    per_head = second_scale.shape[0]
    val_w = head_gain.shape[0]
    head_w = attn_w // per_head
    tok_b, cols = routed_rows.shape
    route_count = route_ids.shape[1]
    hidden_w = expert_gate.shape[2]
    out_w = out_weight.shape[1]
    n_z = n_ep // lanes
    cap = 2 * tok_b * route_count // n_ep
    slots = n_ep * cap
    vmem = pl.BlockSpec(memory_space=pltpu.VMEM)
    hbm = pl.BlockSpec(memory_space=pl.ANY)
    dma = pltpu.SemaphoreType.DMA
    return pl.pallas_call(
        functools.partial(layer_kernel, n_ep, n_tp),
        out_shape=(
            jax.ShapeDtypeStruct((n_tok, out_w), bf16),
            jax.ShapeDtypeStruct((tok_b, out_w), bf16),
        ),
        in_specs=[
            pl.BlockSpec(memory_space=pltpu.SMEM),
            hbm,
            hbm,
            hbm,
            vmem,
            hbm,
            hbm,
            vmem,
            vmem,
            vmem,
            hbm,
            hbm,
            hbm,
        ],
        out_specs=(vmem, vmem),
        scratch_shapes=[
            pltpu.VMEM((n_tok, attn_w), bf16),
            pltpu.VMEM((per_head, 2 * n_tok, head_w), bf16),
            pltpu.VMEM((n_ep, n_tok, attn_w), bf16),
            pltpu.VMEM((n_ep, n_tok, value_rows.shape[1]), bf16),
            pltpu.VMEM((n_ep, tok_b, cols), bf16),
            pltpu.VMEM((n_ep, 8, tok_b), jnp.int32),
            pltpu.VMEM((n_tp, slots, cols), bf16),
            pltpu.VMEM((slots, n_tp * cols), bf16),
            pltpu.VMEM((n_tp, slots, hidden_w), bf16),
            pltpu.VMEM((slots, out_w), bf16),
            pltpu.VMEM((slots, out_w), bf16),
            pltpu.VMEM((n_tp, n_tok, per_head * val_w), bf16),
            pltpu.VMEM((route_count, tok_b, slots), bf16),
            pltpu.VMEM((per_head, 2 * n_tok, val_w), f32),
            pltpu.VMEM((per_head, 2 * n_tok, 1), f32),
            pltpu.VMEM((per_head, 2 * n_tok, 1), f32),
            pltpu.VMEM(expert_gate.shape[1:], bf16),
            pltpu.VMEM(expert_up.shape[1:], bf16),
            pltpu.VMEM(expert_down.shape[1:], bf16),
            pltpu.VMEM(out_weight.shape, bf16),
            dma((4,)),
            dma((4,)),
            dma((n_z,)),
            dma((n_z,)),
            dma((n_z,)),
            dma((n_ep,)),
            dma((n_ep,)),
            dma((n_ep,)),
            dma((2, n_z)),
            dma((2, n_z)),
            dma((2, n_ep)),
            dma((n_tp, 4)),
            dma((n_tp, 4)),
            dma((n_tp, 4)),
            dma((n_tp, 4)),
            dma((n_tp, 2)),
            dma((n_tp, 2)),
            dma((n_ep,)),
            dma((n_ep,)),
        ],
        compiler_params=pltpu.CompilerParams(
            collective_id=0, has_side_effects=True, vmem_limit_bytes=66000000
        ),
    )(
        second_scale,
        query_rows,
        key_rows,
        value_rows,
        head_gain.reshape(1, -1),
        out_weight,
        routed_rows,
        norm_gain.reshape(1, -1),
        route_ids.T,
        route_weight.T,
        expert_gate,
        expert_up,
        expert_down,
    )


def solution(mesh):
    placed = (
        P("ep", "tp"),
        P("ep", "tp"),
        P("ep", "tp"),
        P("tp"),
        P(),
        P(None, "tp"),
        P("ep", "tp"),
        P(),
        P("ep", None),
        P("ep", None),
        P("ep", None, "tp"),
        P("ep", None, "tp"),
        P("ep", None, "tp"),
    )
    return jax.shard_map(
        functools.partial(per_device, mesh.shape["ep"], mesh.shape["tp"]),
        mesh=mesh,
        in_specs=placed,
        out_specs=(P("ep", "tp"), P("ep", "tp")),
        check_vma=False,
    )
```

```python
import functools

import jax
import jax.numpy as jnp
from jax import lax
from jax.experimental import pallas as pl
from jax.experimental.pallas import tpu as pltpu
from jax.sharding import PartitionSpec as P

eps = 1e-06
head_factor = 0.8
neg_big = -1e30
lanes = 2
f32 = jnp.float32
bf16 = jnp.bfloat16


def dot(a, b):
    return jnp.dot(a, b, preferred_element_type=f32)


def layer_kernel(
    n_ep,
    n_tp,
    scale_ref,
    q_hbm,
    k_hbm,
    v_hbm,
    gain_ref,
    wo_hbm,
    rows_hbm,
    norm_ref,
    ids_ref,
    route_w_ref,
    wg_hbm,
    wu_hbm,
    wd_hbm,
    mixer_ref,
    mix_ref,
    q_in,
    q_two,
    k_all,
    v_all,
    rows_all,
    ids_all,
    arr,
    normed,
    hid_all,
    out_e,
    ret,
    head_all,
    spread,
    acc,
    run_max,
    run_sum,
    wg,
    wu,
    wd,
    wo,
    local_sem,
    weight_sem,
    rows_up,
    rows_down,
    rows_side,
    rows_recv,
    ids_send,
    ids_recv,
    kv_up,
    kv_side,
    kv_recv,
    arr_send,
    arr_recv,
    hid_send,
    hid_recv,
    head_send,
    head_recv,
    ret_send,
    ret_recv,
):
    e = lax.axis_index("ep")
    t = lax.axis_index("tp")
    n_z = n_ep // lanes
    z = lax.div(e, lanes)
    c = lax.rem(e, lanes)
    partner = z * lanes + (1 - c)
    n_tok = q_in.shape[0]
    tok_b = rows_all.shape[1]
    per_head = acc.shape[0]
    head_w = q_two.shape[2]
    val_w = acc.shape[2]
    slots, out_w = ret.shape
    cap = slots // n_ep
    half = n_z // 2
    cols = arr.shape[2]
    hidden_w = hid_all.shape[2]
    route_count = ids_ref.shape[0]

    def remote(src, dst, send, recv, ep_to, tp_to):
        return pltpu.make_async_remote_copy(
            src_ref=src,
            dst_ref=dst,
            send_sem=send,
            recv_sem=recv,
            device_id=(ep_to, tp_to),
            device_id_type=pl.DeviceIdType.MESH,
        )

    loads = [
        pltpu.make_async_copy(rows_hbm, rows_all.at[e], local_sem.at[0]),
        pltpu.make_async_copy(k_hbm, k_all.at[e], local_sem.at[1]),
        pltpu.make_async_copy(v_hbm, v_all.at[e], local_sem.at[2]),
        pltpu.make_async_copy(q_hbm, q_in, local_sem.at[3]),
    ]
    for load in loads:
        load.start()
    ids_all[e, pl.ds(0, route_count)] = ids_ref[...]
    weights = [
        pltpu.make_async_copy(wg_hbm.at[0], wg, weight_sem.at[0]),
        pltpu.make_async_copy(wu_hbm.at[0], wu, weight_sem.at[1]),
        pltpu.make_async_copy(wd_hbm.at[0], wd, weight_sem.at[2]),
        pltpu.make_async_copy(wo_hbm, wo, weight_sem.at[3]),
    ]

    barrier = pltpu.get_barrier_semaphore()

    def greet_ep(i, carry):
        to = lax.rem(e + i, n_ep)
        pl.semaphore_signal(barrier, inc=1, device_id=(to, t), device_id_type=pl.DeviceIdType.MESH)
        return carry

    def greet_tp(i, carry):
        to = lax.rem(t + i, n_tp)
        pl.semaphore_signal(barrier, inc=1, device_id=(e, to), device_id_type=pl.DeviceIdType.MESH)
        return carry

    lax.fori_loop(1, n_ep, greet_ep, 0)
    lax.fori_loop(1, n_tp, greet_tp, 0)
    pl.semaphore_wait(barrier, n_ep - 1 + n_tp - 1)
    for load in loads:
        load.wait()

    def ids_copy(to):
        return remote(ids_all.at[e], ids_all.at[e], ids_send.at[to], ids_recv.at[e], to, t)

    def ids_arrival(b):
        return remote(ids_all.at[b], ids_all.at[b], ids_send.at[b], ids_recv.at[b], b, t)

    def rows_copy(block, send, to):
        return remote(rows_all.at[block], rows_all.at[block], send, rows_recv.at[block], to, t)

    def rows_copy_up(j):
        return rows_copy(j * lanes + c, rows_up.at[j], lax.rem(e + lanes, n_ep))

    def rows_copy_down(j):
        return rows_copy(j * lanes + c, rows_down.at[j], lax.rem(e + n_ep - lanes, n_ep))

    def rows_copy_side(j):
        return rows_copy(j * lanes + c, rows_side.at[j], partner)

    def kv_copies(j, sems, to):
        block = j * lanes + c
        return [
            remote(ref.at[block], ref.at[block], sems.at[i, j], kv_recv.at[i, block], to, t)
            for i, ref in enumerate((k_all, v_all))
        ]

    def kv_copies_up(j):
        return kv_copies(j, kv_up, lax.rem(e + lanes, n_ep))

    def kv_copies_side(j):
        return kv_copies(j, kv_side, partner)

    def kv_wait(block):
        for i, ref in enumerate((k_all, v_all)):
            remote(
                ref.at[block], ref.at[block], kv_up.at[i, 0], kv_recv.at[i, block], partner, t
            ).wait_recv()

    square = n_tp == 4
    across = t + 1 - 2 * lax.rem(t, 2)
    along = lax.rem(t + 2, n_tp)
    corner = n_tp - 1 - t

    def piece(buf, source, i, units):
        step = buf.shape[1] // (2 * units)
        return buf.at[source, pl.ds(i * step, step)]

    def tp_copy(buf, sems, units, source, i, row, to):
        ref = piece(buf, source, i, units)
        return remote(ref, ref, sems[0].at[row, i], sems[1].at[source, i], e, to)

    def tp_peers(work):
        def one(i, carry):
            to = lax.rem(t + i, n_tp)
            work(to, to)
            return carry

        if square:
            work(across, 0)
            work(along, 1)
        else:
            lax.fori_loop(1, n_tp, one, 0)

    def tp_send(buf, sems, units, unit):
        for i in (2 * unit, 2 * unit + 1):
            tp_peers(lambda to, row: tp_copy(buf, sems, units, t, i, row, to).start())

    def tp_hand_on(buf, sems, units, unit):
        if square:
            i = 2 * unit
            tp_copy(buf, sems, units, across, i, 2, across).wait_recv()
            tp_copy(buf, sems, units, across, i, 2, along).start()
            tp_copy(buf, sems, units, along, i + 1, 2, along).wait_recv()
            tp_copy(buf, sems, units, along, i + 1, 2, across).start()

    def tp_arrive(buf, sems, units, unit):
        i = 2 * unit
        if square:
            for source, at in ((across, i + 1), (along, i), (corner, i), (corner, i + 1)):
                tp_copy(buf, sems, units, source, at, 2, source).wait_recv()
        else:
            for at in (i, i + 1):
                tp_peers(lambda to, row: tp_copy(buf, sems, units, to, at, row, to).wait_recv())

    def tp_drain(buf, sems, units):
        for i in range(2 * units):
            tp_peers(lambda to, row: tp_copy(buf, sems, units, t, i, row, to).wait_send())
            if square:
                source, to = (across, along) if i % 2 == 0 else (along, across)
                tp_copy(buf, sems, units, source, i, 2, to).wait_send()

    arr_sems = (arr_send, arr_recv)
    hid_sems = (hid_send, hid_recv)
    head_sems = (head_send, head_recv)

    def unit_of(j):
        return lax.rem(lax.div(j, half) + lax.div(z, half), 2)

    def first_slot(j, side):
        return pl.multiple_of(((unit_of(j) * 2 + side) * half + lax.rem(j, half)) * cap, cap)

    def ret_part(b):
        return ret.at[pl.ds(pl.multiple_of(b * cap, cap), cap)]

    def ret_copy(j, side):
        to = j * lanes + (c if side == 0 else 1 - c)
        return remote(
            out_e.at[pl.ds(first_slot(j, side), cap)],
            ret_part(e),
            ret_send.at[to],
            ret_recv.at[e],
            to,
            t,
        )

    def ret_each(unit, work):
        def one(i, carry):
            j = lax.rem(lax.div(z, half) + unit, 2) * half + i
            if unit == 0:

                @pl.when(j != z)
                def _():
                    work(ret_copy(j, 0))

            else:
                work(ret_copy(j, 0))
            work(ret_copy(j, 1))
            return carry

        lax.fori_loop(0, half, one, 0)

    def ret_arrival(b):
        return remote(ret_part(b), ret_part(b), ret_send.at[b], ret_recv.at[b], b, t)

    def each_ep(work):
        def one(i, carry):
            work(lax.rem(e + i, n_ep))
            return carry

        lax.fori_loop(1, n_ep, one, 0)

    each_ep(lambda to: ids_copy(to).start())

    def pick(block, j, side):
        ids = ids_all[block]
        hit = (ids[0:1] == e).astype(f32)
        for k in range(1, route_count):
            hit = hit + (ids[k : k + 1] == e).astype(f32)
        before = (
            lax.broadcasted_iota(jnp.int32, (tok_b, tok_b), 0)
            < lax.broadcasted_iota(jnp.int32, (tok_b, tok_b), 1)
        ).astype(bf16)
        ranks = dot(jnp.broadcast_to(hit, (16, tok_b)).astype(bf16), before)[0:1]
        slot = lax.broadcasted_iota(jnp.int32, (cap, tok_b), 0).astype(f32)
        chosen = jnp.where((slot == ranks) & (hit > 0.5), 1.0, 0.0).astype(bf16)
        start = first_slot(j, side)
        i = unit_of(j) * 2 + side
        arr[t, pl.ds(start, cap)] = dot(chosen, rows_all[block]).astype(bf16)
        part = arr.at[t, pl.ds(start, cap)]
        tp_peers(
            lambda to, row: remote(
                part, part, arr_send.at[row, i], arr_recv.at[t, i], e, to
            ).start()
        )

    def rows_step(s, carry):
        low, high = z - s, z + s

        @pl.when((s > 0) & (low >= 0))
        def _():
            rows_copy_down(low).wait_recv()

        @pl.when((low >= 0) & (z + 1 < n_z))
        def _():
            rows_copy_up(low).start()

        @pl.when((s > 0) & (high < n_z))
        def _():
            rows_copy_up(high).wait_recv()

        @pl.when((high < n_z) & (z > 0))
        def _():
            rows_copy_down(high).start()

        @pl.when((s == z) & (z + 1 < n_z))
        def _():
            for copy in kv_copies_up(z):
                copy.start()

        @pl.when((s == z) & (c == 0))
        def _():
            for copy in kv_copies_side(z):
                copy.start()

        @pl.when(low >= 0)
        def _():
            rows_copy_side(low).start()

        @pl.when((s > 0) & (high < n_z))
        def _():
            rows_copy_side(high).start()

        def take(j):
            mine, other = j * lanes + c, j * lanes + (1 - c)

            @pl.when(j != z)
            def _():
                ids_arrival(mine).wait_recv()

            pick(mine, j, 0)
            ids_arrival(other).wait_recv()
            rows_copy(other, rows_side.at[j], partner).wait_recv()
            pick(other, j, 1)

        @pl.when(low >= 0)
        def _():
            take(low)

        @pl.when((s > 0) & (high < n_z))
        def _():
            take(high)

        return carry

    lax.fori_loop(0, n_z, rows_step, 0)
    for weight in weights:
        weight.start()
    tp_hand_on(arr, arr_sems, 2, 0)

    lane = lax.broadcasted_iota(jnp.int32, (n_tok, head_w), 1)

    def split_maps(h, carry):
        scaled = q_in[:, pl.ds(pl.multiple_of(h * head_w, head_w), head_w)].astype(f32) * (
            (head_w // 2) ** -0.5
        )
        q_two[h, pl.ds(0, n_tok)] = jnp.where(lane < head_w // 2, scaled, 0.0).astype(bf16)
        q_two[h, pl.ds(n_tok, n_tok)] = jnp.where(lane < head_w // 2, 0.0, scaled).astype(bf16)
        return carry

    lax.fori_loop(0, per_head, split_maps, 0)

    def attend(block, own):
        def one(h, carry):
            keys = k_all[block, :, pl.ds(pl.multiple_of(h * head_w, head_w), head_w)]
            values = v_all[block, :, pl.ds(pl.multiple_of(h * val_w, val_w), val_w)]
            parts = [pl.ds(m * n_tok, n_tok) for m in range(2)]
            held = []
            if not own:
                held = [(run_max[h, part], run_sum[h, part], acc[h, part]) for part in parts]
            results = []
            for m, part in enumerate(parts):
                scores = lax.dot_general(
                    q_two[h, part], keys, (((1,), (1,)), ((), ())), preferred_element_type=f32
                )
                if own:
                    scores = jnp.where(
                        lax.broadcasted_iota(jnp.int32, (n_tok, n_tok), 0)
                        >= lax.broadcasted_iota(jnp.int32, (n_tok, n_tok), 1),
                        scores,
                        neg_big,
                    )
                top = jnp.max(scores, axis=-1, keepdims=True)
                if not own:
                    old, old_sum, old_acc = held[m]
                    top = jnp.maximum(old, top)
                shares = jnp.exp(scores - top)
                total = jnp.sum(shares, axis=-1, keepdims=True)
                update = dot(shares.astype(bf16), values)
                if not own:
                    shrink = jnp.exp(old - top)
                    total = total + old_sum * shrink
                    update = update + old_acc * shrink
                results.append((top, total, update))
            for part, (top, total, update) in zip(parts, results):
                run_max[h, part] = top
                run_sum[h, part] = total
                acc[h, part] = update
            return carry

        lax.fori_loop(0, per_head, one, 0)

    attend(e, True)

    @pl.when(c == 1)
    def _():
        kv_wait(partner)
        attend(partner, False)

    tp_hand_on(arr, arr_sems, 2, 1)

    def kv_pass(s, carry):
        j = z - s

        @pl.when(j >= 0)
        def _():
            kv_wait(j * lanes + c)

            @pl.when(z + 1 < n_z)
            def _():
                for copy in kv_copies_up(j):
                    copy.start()

            for copy in kv_copies_side(j):
                copy.start()

        return carry

    def kv_attend(s, carry):
        j = z - s

        @pl.when(j >= 0)
        def _():
            attend(j * lanes + c, False)
            kv_wait(j * lanes + (1 - c))
            attend(j * lanes + (1 - c), False)

        return carry

    lax.fori_loop(1, 2, kv_pass, 0)

    for weight in weights:
        weight.wait()
    unit_rows = slots // 2
    n_rows = min(unit_rows, 64)
    tile_f = min(hidden_w, 256)

    def expert_in(unit):
        tp_arrive(arr, arr_sems, 2, unit)

        def norm_step(i, carry):
            part = pl.ds(pl.multiple_of(unit * unit_rows + i * n_rows, n_rows), n_rows)
            squares = jnp.zeros((n_rows, 1), f32)
            for p in range(n_tp):
                x = arr[p, part].astype(f32)
                squares = squares + jnp.sum(x * x, axis=-1, keepdims=True)
            factor = lax.rsqrt(squares / (n_tp * cols) + eps)
            for p in range(n_tp):
                where = pl.ds(p * cols, cols)
                normed[part, where] = (
                    arr[p, part].astype(f32) * factor * norm_ref[0:1, where]
                ).astype(bf16)
            return carry

        lax.fori_loop(0, unit_rows // n_rows, norm_step, 0)
        rows = pl.ds(unit * unit_rows, unit_rows)

        def gate_step(i, carry):
            where = pl.ds(pl.multiple_of(i * tile_f, tile_f), tile_f)
            gate = dot(normed[rows], wg[:, where])
            up = dot(normed[rows], wu[:, where])
            hid_all[t, rows, where] = (gate / (1.0 + jnp.exp(-gate)) * up).astype(bf16)
            return carry

        lax.fori_loop(0, hidden_w // tile_f, gate_step, 0)
        tp_send(hid_all, hid_sems, 2, unit)

    expert_in(0)
    expert_in(1)
    @pl.when(z + 1 < n_z)
    def _():
        lax.fori_loop(2, n_z - 1, kv_pass, 0)

    lax.fori_loop(1, 2, kv_attend, 0)

    tp_hand_on(hid_all, hid_sems, 2, 0)
    tp_hand_on(hid_all, hid_sems, 2, 1)
    tile_o = min(out_w, 256)

    def expert_out(unit):
        tp_arrive(hid_all, hid_sems, 2, unit)
        rows = pl.ds(unit * unit_rows, unit_rows)

        def down_step(i, carry):
            where = pl.ds(pl.multiple_of(i * tile_o, tile_o), tile_o)
            total = dot(hid_all[0, rows], wd[pl.ds(0, hidden_w), where])
            for p in range(1, n_tp):
                total = total + dot(hid_all[p, rows], wd[pl.ds(p * hidden_w, hidden_w), where])
            out_e[rows, where] = total.astype(bf16)
            return carry

        lax.fori_loop(0, out_w // tile_o, down_step, 0)
        ret_each(unit, lambda copy: copy.start())

    expert_out(0)
    expert_out(1)
    ret[pl.ds(pl.multiple_of(e * cap, cap), cap)] = out_e[pl.ds(first_slot(z, 0), cap)]

    def kv_late(s, carry):
        @pl.when(z + 1 == n_z)
        def _():
            kv_pass(s, 0)

        return kv_attend(s, carry)

    lax.fori_loop(2, n_z, kv_late, 0)

    def head_step(h, carry):
        first = acc[h, pl.ds(0, n_tok)] / run_sum[h, pl.ds(0, n_tok)]
        second = acc[h, pl.ds(n_tok, n_tok)] / run_sum[h, pl.ds(n_tok, n_tok)]
        mixed = first - scale_ref[h] * second
        mean_sq = jnp.mean(mixed * mixed, axis=-1, keepdims=True)
        head_all[t, :, pl.ds(pl.multiple_of(h * val_w, val_w), val_w)] = (
            mixed * lax.rsqrt(mean_sq + eps) * gain_ref[0:1] * head_factor
        ).astype(bf16)
        return carry

    lax.fori_loop(0, per_head, head_step, 0)
    tp_send(head_all, head_sems, 1, 0)

    row_of = lax.broadcasted_iota(jnp.int32, (tok_b, tok_b), 0)
    col_of = lax.broadcasted_iota(jnp.int32, (tok_b, tok_b), 1)

    def column(row):
        return jnp.sum(
            jnp.where(row_of == col_of, row.astype(f32), 0.0), axis=1, keepdims=True
        )

    shares = []
    for k in range(route_count):
        ids = column(ids_ref[k : k + 1])
        same = jnp.zeros((tok_b, tok_b), f32)
        for other in range(route_count):
            same = same + (ids_ref[other : other + 1].astype(f32) == ids).astype(f32)
        ranks = jnp.sum(jnp.where(col_of < row_of, same, 0.0), axis=1, keepdims=True)
        slot = lax.broadcasted_iota(jnp.int32, (tok_b, slots), 1).astype(f32)
        spread[k] = jnp.where(slot == ids * cap + ranks, 1.0, 0.0).astype(bf16)
        shares.append(column(route_w_ref[k : k + 1]))

    tp_hand_on(head_all, head_sems, 1, 0)
    tp_arrive(head_all, head_sems, 1, 0)
    heads_w = head_all.shape[2]

    def mixer_step(i, carry):
        where = pl.ds(pl.multiple_of(i * tile_o, tile_o), tile_o)
        total = dot(head_all[0], wo[pl.ds(0, heads_w), where])
        for p in range(1, n_tp):
            total = total + dot(head_all[p], wo[pl.ds(p * heads_w, heads_w), where])
        mixer_ref[:, where] = total.astype(bf16)
        return carry

    lax.fori_loop(0, out_w // tile_o, mixer_step, 0)

    each_ep(lambda b: ret_arrival(b).wait_recv())
    tile_m = min(out_w, 256)
    for start in range(0, out_w, tile_m):
        where = pl.ds(start, tile_m)
        total = shares[0] * dot(spread[0], ret[:, where])
        for k in range(1, route_count):
            total = total + shares[k] * dot(spread[k], ret[:, where])
        mix_ref[:, where] = total.astype(bf16)

    each_ep(lambda to: ids_copy(to).wait_send())
    for unit in range(2):
        ret_each(unit, lambda copy: copy.wait_send())
    tp_drain(arr, arr_sems, 2)
    tp_drain(hid_all, hid_sems, 2)
    tp_drain(head_all, head_sems, 1)

    def drain(j, carry):
        rows_copy_side(j).wait_send()

        @pl.when((j <= z) & (z + 1 < n_z))
        def _():
            rows_copy_up(j).wait_send()
            for copy in kv_copies_up(j):
                copy.wait_send()

        @pl.when((j >= z) & (z > 0))
        def _():
            rows_copy_down(j).wait_send()

        @pl.when((j < z) | ((j == z) & (c == 0)))
        def _():
            for copy in kv_copies_side(j):
                copy.wait_send()

        return carry

    lax.fori_loop(0, n_z, drain, 0)


def per_device(
    n_ep,
    n_tp,
    query_rows,
    key_rows,
    value_rows,
    second_scale,
    head_gain,
    out_weight,
    routed_rows,
    norm_gain,
    route_ids,
    route_weight,
    expert_gate,
    expert_up,
    expert_down,
):
    n_tok, attn_w = query_rows.shape
    per_head = second_scale.shape[0]
    val_w = head_gain.shape[0]
    head_w = attn_w // per_head
    tok_b, cols = routed_rows.shape
    route_count = route_ids.shape[1]
    hidden_w = expert_gate.shape[2]
    out_w = out_weight.shape[1]
    n_z = n_ep // lanes
    cap = 2 * tok_b * route_count // n_ep
    slots = n_ep * cap
    vmem = pl.BlockSpec(memory_space=pltpu.VMEM)
    hbm = pl.BlockSpec(memory_space=pl.ANY)
    dma = pltpu.SemaphoreType.DMA
    return pl.pallas_call(
        functools.partial(layer_kernel, n_ep, n_tp),
        out_shape=(
            jax.ShapeDtypeStruct((n_tok, out_w), bf16),
            jax.ShapeDtypeStruct((tok_b, out_w), bf16),
        ),
        in_specs=[
            pl.BlockSpec(memory_space=pltpu.SMEM),
            hbm,
            hbm,
            hbm,
            vmem,
            hbm,
            hbm,
            vmem,
            vmem,
            vmem,
            hbm,
            hbm,
            hbm,
        ],
        out_specs=(vmem, vmem),
        scratch_shapes=[
            pltpu.VMEM((n_tok, attn_w), bf16),
            pltpu.VMEM((per_head, 2 * n_tok, head_w), bf16),
            pltpu.VMEM((n_ep, n_tok, attn_w), bf16),
            pltpu.VMEM((n_ep, n_tok, value_rows.shape[1]), bf16),
            pltpu.VMEM((n_ep, tok_b, cols), bf16),
            pltpu.VMEM((n_ep, 8, tok_b), jnp.int32),
            pltpu.VMEM((n_tp, slots, cols), bf16),
            pltpu.VMEM((slots, n_tp * cols), bf16),
            pltpu.VMEM((n_tp, slots, hidden_w), bf16),
            pltpu.VMEM((slots, out_w), bf16),
            pltpu.VMEM((slots, out_w), bf16),
            pltpu.VMEM((n_tp, n_tok, per_head * val_w), bf16),
            pltpu.VMEM((route_count, tok_b, slots), bf16),
            pltpu.VMEM((per_head, 2 * n_tok, val_w), f32),
            pltpu.VMEM((per_head, 2 * n_tok, 1), f32),
            pltpu.VMEM((per_head, 2 * n_tok, 1), f32),
            pltpu.VMEM(expert_gate.shape[1:], bf16),
            pltpu.VMEM(expert_up.shape[1:], bf16),
            pltpu.VMEM(expert_down.shape[1:], bf16),
            pltpu.VMEM(out_weight.shape, bf16),
            dma((4,)),
            dma((4,)),
            dma((n_z,)),
            dma((n_z,)),
            dma((n_z,)),
            dma((n_ep,)),
            dma((n_ep,)),
            dma((n_ep,)),
            dma((2, n_z)),
            dma((2, n_z)),
            dma((2, n_ep)),
            dma((n_tp, 4)),
            dma((n_tp, 4)),
            dma((n_tp, 4)),
            dma((n_tp, 4)),
            dma((n_tp, 2)),
            dma((n_tp, 2)),
            dma((n_ep,)),
            dma((n_ep,)),
        ],
        compiler_params=pltpu.CompilerParams(
            collective_id=0, has_side_effects=True, vmem_limit_bytes=66000000
        ),
    )(
        second_scale,
        query_rows,
        key_rows,
        value_rows,
        head_gain.reshape(1, -1),
        out_weight,
        routed_rows,
        norm_gain.reshape(1, -1),
        route_ids.T,
        route_weight.T,
        expert_gate,
        expert_up,
        expert_down,
    )


def solution(mesh):
    placed = (
        P("ep", "tp"),
        P("ep", "tp"),
        P("ep", "tp"),
        P("tp"),
        P(),
        P(None, "tp"),
        P("ep", "tp"),
        P(),
        P("ep", None),
        P("ep", None),
        P("ep", None, "tp"),
        P("ep", None, "tp"),
        P("ep", None, "tp"),
    )
    return jax.shard_map(
        functools.partial(per_device, mesh.shape["ep"], mesh.shape["tp"]),
        mesh=mesh,
        in_specs=placed,
        out_specs=(P("ep", "tp"), P("ep", "tp")),
        check_vma=False,
    )
```
